32 devices in a mesh: sp: 8 (over z, y), tp: 4 (over x, core).
Axes of the slice: x: 2, y: 2, z: 4, core: 2. Of those that a mesh axis runs over, the one named last changes fastest.
Arguments:
- tokens: bfloat16 [4, 512, 2048], P(None, ('sp', 'tp')), may hold values from -6 to 6
- in_gain: float32 [2048], replicated, may hold values from 0.1 to 1.9
- gate_weight: bfloat16 [2048, 1024], P(None, 'tp'), may hold values from -0.125 to 0.125
- input_weight: bfloat16 [2048, 1024], P(None, 'tp'), may hold values from -0.125 to 0.125
- key_weight: bfloat16 [2048, 512], P(None, 'tp'), may hold values from -0.125 to 0.125
- query_weight: bfloat16 [2048, 512], P(None, 'tp'), may hold values from -0.125 to 0.125
- step_weight: bfloat16 [2048, 16], replicated, may hold values from -0.125 to 0.125
- conv_input: float32 [4, 1024], P(None, 'tp'), may hold values from -3 to 3
- conv_key: float32 [4, 512], P(None, 'tp'), may hold values from -3 to 3
- conv_query: float32 [4, 512], P(None, 'tp'), may hold values from -3 to 3
- step_bias: float32 [16], P('tp'), may hold values from -5 to 1
- decay_rate: float32 [16], P('tp'), may hold values from 0 to 1, as said below
- decay_extra: float32 [4, 16, 512], P(None, 'tp', 'sp'), may hold values from -0.7 to 0, as said below
- out_gain: float32 [1024], P('tp'), may hold values from 0.1 to 1.9
- out_weight: bfloat16 [1024, 2048], replicated, may hold values from -0.1875 to 0.1875
Outputs:
- output: bfloat16 [4, 512, 2048], P(None, ('sp', 'tp'))
The draws below stay inside these ranges and needn't reach their ends.
Inputs may be any that keep to these rules, and one draw needn't show every extreme that they name: `decay_rate`: one positive rate a head. `decay_extra`: never positive.
All inputs are finite; a program needn't handle non-finite values.
Results may differ from the reference program's by a relative error of at most 0.0072.
Values may be sent and summed in bfloat16 or wider, within the bound.
A program may use at most 128 MiB of HBM per device.

```python
import jax
import jax.numpy as jnp
from jax import lax

D = 2048
HEAD_TOTAL = 16
HEAD_DIM = 64
GROUPS = 8
STATE = 64
CONV = 4
BLOCK = 64
SEQUENCE_TOTAL = 4
INNER = 1024
LEN = 512


def fast_heads(key):
    picks = jax.random.randint(jax.random.fold_in(key, 7), (HEAD_TOTAL,), 0, 8)
    return picks < 4


def draw_decay_rate(key, part):
    is_fast = fast_heads(key)
    unit_draw = jax.random.uniform(jax.random.fold_in(key, 11), (HEAD_TOTAL,), jnp.float32)
    fast_rate = jnp.exp(jnp.log(1.0 / 60.0) + unit_draw * jnp.log(60.0 / 25.0))
    slow_rate = jnp.exp(jnp.log(8.0) + unit_draw * jnp.log(20.0 / 8.0)) / LEN
    return jnp.where(is_fast, fast_rate, slow_rate).astype(jnp.float32)


def draw_step_bias(key, part):
    is_fast = fast_heads(key)
    unit_draw = jax.random.uniform(jax.random.fold_in(key, 13), (HEAD_TOTAL,), jnp.float32)
    return jnp.where(is_fast, unit_draw - 0.5, unit_draw - 4.5).astype(jnp.float32)


def draw_decay_extra(key, part):
    block_total = LEN // BLOCK
    unit_draw = jax.random.uniform(jax.random.fold_in(key, 17), (SEQUENCE_TOTAL, HEAD_TOTAL, block_total), jnp.float32)
    factor = jnp.exp(jnp.log(0.1) + unit_draw * jnp.log(8.0)) / LEN
    block_displacement = -jnp.repeat(factor, BLOCK, axis=2)
    first_spot = jax.random.randint(jax.random.fold_in(key, 19), (SEQUENCE_TOTAL, HEAD_TOTAL, 1), 0, LEN)
    spot_offset = jax.random.randint(jax.random.fold_in(key, 29), (SEQUENCE_TOTAL, HEAD_TOTAL, 1), 1, LEN)
    second_spot = (first_spot + spot_offset) % LEN
    spots = jnp.concatenate([first_spot, second_spot], axis=2)
    segment_lengths = jax.random.uniform(jax.random.fold_in(key, 23), (SEQUENCE_TOTAL, HEAD_TOTAL, 2), jnp.float32, 0.22, 0.69)
    positions = jnp.arange(LEN)[None, None, :, None]
    matching_count = positions == spots[:, :, None, :]
    token_segments = jnp.sum(jnp.where(matching_count, segment_lengths[:, :, None, :], 0.0), axis=3)
    return (block_displacement - token_segments).astype(jnp.float32)


def shard_levels(rng, dims, shards, low, top_value):
    factor_of, own = 1.0, jax.random.fold_in(rng, 6)
    for dim, shards_of in shards:
        draws = jnp.exp(jax.random.uniform(jax.random.fold_in(own, dim), (shards_of,), jnp.float32, low / len(shards), top_value / len(shards)))
        factor_of = factor_of * jnp.repeat(draws, dims[dim] // shards_of).reshape([-1 if axis == dim else 1 for axis in range(len(dims))])
    return factor_of


def scatter_about(rng, extent, deviation, reach, pieces=(), dtype=jnp.bfloat16):
    values = deviation * jax.random.normal(rng, extent, jnp.float32)
    if pieces:
        values = values * shard_levels(rng, extent, pieces, -0.22, 0.18)
    return jnp.clip(values, -reach, reach).astype(dtype)


def setup_inputs(seed: int = 0) -> dict:
    key_of = jax.random.split(jax.random.key(seed), 16)
    return {
        "tokens": scatter_about(key_of[0], (SEQUENCE_TOTAL, LEN, D), 1.0, 6.0, ((1, 32),)),
        "in_gain": jnp.clip(1.0 + 0.18 * jax.random.normal(key_of[1], (D,), jnp.float32), 0.1, 1.9),
        "gate_weight": scatter_about(key_of[2], (D, INNER), D ** -0.5, 0.125, ((1, 4),)),
        "input_weight": scatter_about(key_of[3], (D, INNER), D ** -0.5, 0.125, ((1, 4),)),
        "key_weight": scatter_about(key_of[4], (D, GROUPS * STATE), D ** -0.5, 0.125, ((1, 4),)),
        "query_weight": scatter_about(key_of[5], (D, GROUPS * STATE), D ** -0.5, 0.125, ((1, 4),)),
        "step_weight": scatter_about(key_of[6], (D, HEAD_TOTAL), D ** -0.5, 0.125),
        "conv_input": scatter_about(key_of[7], (CONV, INNER), CONV ** -0.5, 3.0, ((1, 4),), jnp.float32),
        "conv_key": scatter_about(key_of[8], (CONV, GROUPS * STATE), CONV ** -0.5, 3.0, ((1, 4),), jnp.float32),
        "conv_query": scatter_about(key_of[9], (CONV, GROUPS * STATE), CONV ** -0.5, 3.0, ((1, 4),), jnp.float32),
        "step_bias": draw_step_bias(jax.random.fold_in(key_of[15], 71), 0),
        "decay_rate": draw_decay_rate(jax.random.fold_in(key_of[15], 71), 0),
        "decay_extra": draw_decay_extra(jax.random.fold_in(key_of[15], 71), 0),
        "out_gain": jnp.clip(1.0 + 0.18 * jax.random.normal(key_of[13], (INNER,), jnp.float32), 0.1, 1.9),
        "out_weight": scatter_about(key_of[14], (INNER, D), INNER ** -0.5, 0.1875),
    }


NORM_EPS = 1e-06
PRECISE = lax.Precision.HIGHEST

def rms_rows(values, gain_row):
    mean_sq = lax.optimization_barrier(jnp.mean(values * values, axis=-1, keepdims=True))
    return values * lax.rsqrt(mean_sq + NORM_EPS) * gain_row

def causal_blend(rim_rows, local_rows, weights):
    length = local_rows.shape[1]
    padded = jnp.concatenate([rim_rows, local_rows], axis=1).astype(jnp.float32)
    summed_rows = padded[:, 0:length, :] * weights[0]
    for offset in range(1, weights.shape[0]):
        summed_rows = summed_rows + padded[:, offset:offset + length, :] * weights[offset]
    return jax.nn.silu(summed_rows)

def reference(tokens, in_gain, gate_weight, input_weight, key_weight, query_weight, step_weight, conv_input, conv_key, conv_query, step_bias, decay_rate, decay_extra, out_gain, out_weight):
    ratio_heads = HEAD_TOTAL // GROUPS
    normed = rms_rows(tokens.astype(jnp.float32), in_gain).astype(jnp.bfloat16)
    flat_rows = normed.reshape(SEQUENCE_TOTAL * LEN, D)

    def project(weight_matrix):
        result = jnp.dot(flat_rows, weight_matrix, preferred_element_type=jnp.float32)
        return result.astype(jnp.bfloat16).reshape(SEQUENCE_TOTAL, LEN, weight_matrix.shape[1])
    gate_in = project(gate_weight)
    input_in = project(input_weight)
    key_in = project(key_weight)
    query_in = project(query_weight)
    step_in = project(step_weight)
    rim_inner = jnp.zeros((SEQUENCE_TOTAL, CONV - 1, INNER), jnp.bfloat16)
    rim_state = jnp.zeros((SEQUENCE_TOTAL, CONV - 1, GROUPS * STATE), jnp.bfloat16)
    conv_values = causal_blend(rim_inner, input_in, conv_input)
    conv_keys = causal_blend(rim_state, key_in, conv_key)
    conv_queries = causal_blend(rim_state, query_in, conv_query)
    step_size = jax.nn.softplus(step_in.astype(jnp.float32) + step_bias)
    log_decay = -step_size * decay_rate + jnp.transpose(decay_extra, (0, 2, 1))
    block_count = LEN // BLOCK

    def to_blocks(tensor):
        shaped = tensor.reshape((SEQUENCE_TOTAL, block_count, BLOCK) + tensor.shape[2:])
        return jnp.moveaxis(shaped, 1, 0)
    x_blocks = to_blocks(conv_values.reshape(SEQUENCE_TOTAL, LEN, HEAD_TOTAL, HEAD_DIM) * step_size[..., None])
    b_blocks = to_blocks(conv_keys.reshape(SEQUENCE_TOTAL, LEN, GROUPS, STATE))
    c_blocks = to_blocks(conv_queries.reshape(SEQUENCE_TOTAL, LEN, GROUPS, STATE))
    d_blocks = to_blocks(log_decay)
    causal = jnp.tril(jnp.ones((BLOCK, BLOCK), bool))[None, :, :, None]

    def block_step(passed_recurrence, inputs):
        x_now, b_now, c_now, d_now = inputs
        inside_block = jnp.cumsum(d_now, axis=1)
        spread_log = inside_block[:, :, None, :] - inside_block[:, None, :, :]
        decay_matrix = jnp.where(causal, jnp.exp(jnp.where(causal, spread_log, 0.0)), 0.0)
        scores = jnp.einsum('slgn,stgn->sltg', c_now, b_now, precision=PRECISE)
        scores = jnp.repeat(scores, ratio_heads, axis=3)
        key_heads = jnp.repeat(b_now, ratio_heads, axis=2)
        query_heads = jnp.repeat(c_now, ratio_heads, axis=2)
        inner_part = jnp.einsum('slth,sthp->slhp', scores * decay_matrix, x_now, precision=PRECISE)
        forwarded_portion = jnp.einsum('slhn,shpn->slhp', query_heads, passed_recurrence, precision=PRECISE)
        forwarded_portion = forwarded_portion * jnp.exp(inside_block)[..., None]
        tail_weight = jnp.exp(inside_block[:, -1:, :] - inside_block)
        fresh = jnp.einsum('slhn,slhp->shpn', key_heads, x_now * tail_weight[..., None], precision=PRECISE)
        next_state = jnp.exp(inside_block[:, -1, :])[:, :, None, None] * passed_recurrence + fresh
        return (next_state, inner_part + forwarded_portion)
    start_state = jnp.zeros((SEQUENCE_TOTAL, HEAD_TOTAL, HEAD_DIM, STATE), jnp.float32)
    _, out_blocks = lax.scan(block_step, start_state, (x_blocks, b_blocks, c_blocks, d_blocks))
    heads_out = jnp.moveaxis(out_blocks, 0, 1).reshape(SEQUENCE_TOTAL, LEN, INNER)
    gated = heads_out * jax.nn.silu(gate_in.astype(jnp.float32))
    group_width = ratio_heads * HEAD_DIM
    mixed = rms_rows(gated.reshape(SEQUENCE_TOTAL, LEN, GROUPS, group_width), out_gain.reshape(GROUPS, group_width))
    mixed = mixed.reshape(SEQUENCE_TOTAL * LEN, INNER).astype(jnp.bfloat16)
    output = jnp.dot(mixed, out_weight, preferred_element_type=jnp.float32).astype(jnp.bfloat16)
    return output.reshape(SEQUENCE_TOTAL, LEN, D)
```

```python
import functools

import jax
import jax.numpy as jnp
from jax import lax
from jax.experimental import pallas as pl
from jax.experimental.pallas import tpu as pltpu
from jax.sharding import PartitionSpec as P

HEAD_TOTAL = 16
HEAD_DIM = 64
GROUPS = 8
STATE = 64
CONV = 4
BLOCK = 64


NORM_EPS = 1e-06
PRECISE = lax.Precision.HIGHEST


def from_behind(array, axis, by):
    length = lax.axis_size(axis)
    pairs = [(i, i + by) for i in range(length) if 0 <= i + by < length]
    return lax.ppermute(array, axis, pairs)


def carried_in(array, axis, combine, identity):
    length, place = (lax.axis_size(axis), lax.axis_index(axis))
    everything = jax.tree.map(lambda part: lax.all_gather(part, axis), array)
    start = jax.tree.map(
        lambda part, zero: jnp.broadcast_to(jnp.asarray(zero, part.dtype), part.shape),
        array,
        identity,
    )

    def step(k, before):
        reached = k < place
        new = combine(before, jax.tree.map(lambda part: part[k], everything))
        return jax.tree.map(lambda a, b: jnp.where(reached, a, b), new, before)

    return lax.fori_loop(0, length, step, start)


def rms_rows(values, gain_row):
    mean_sq = jnp.mean(values * values, axis=-1, keepdims=True)
    return values * lax.rsqrt(mean_sq + NORM_EPS) * gain_row


def causal_blend(rim_rows, local_rows, weights):
    length = local_rows.shape[1]
    padded = jnp.concatenate([rim_rows, local_rows], axis=1).astype(jnp.float32)
    summed_rows = padded[:, 0:length, :] * weights[0]
    for offset in range(1, weights.shape[0]):
        summed_rows = summed_rows + padded[:, offset : offset + length, :] * weights[offset]
    return jax.nn.silu(summed_rows)


def local_pass(scaled_x, keys_b, readout_vectors, log_decay):
    seq_count, seg_len, heads_here = (scaled_x.shape[0], scaled_x.shape[1], scaled_x.shape[2])
    blocks_here = seg_len // BLOCK
    ratio_heads = HEAD_TOTAL // GROUPS

    def to_blocks(tensor):
        return tensor.reshape((seq_count, blocks_here, BLOCK) + tensor.shape[2:])

    x_blocks = to_blocks(scaled_x)
    b_blocks = to_blocks(keys_b)
    c_blocks = to_blocks(readout_vectors)
    inside_block = jnp.cumsum(to_blocks(log_decay), axis=2)
    causal = jnp.tril(jnp.ones((BLOCK, BLOCK), bool))[None, None, :, :, None]
    spread_log = inside_block[:, :, :, None, :] - inside_block[:, :, None, :, :]
    decay_matrix = jnp.where(causal, jnp.exp(jnp.where(causal, spread_log, 0.0)), 0.0)
    scores = jnp.einsum("sblgn,sbtgn->sbltg", c_blocks, b_blocks, precision=PRECISE)
    scores = jnp.repeat(scores, ratio_heads, axis=4)
    key_heads = jnp.repeat(b_blocks, ratio_heads, axis=3)
    query_heads = jnp.repeat(c_blocks, ratio_heads, axis=3)
    inner_part = jnp.einsum(
        "sblth,sbthp->sblhp", scores * decay_matrix, x_blocks, precision=PRECISE
    )
    tail_weight = jnp.exp(inside_block[:, :, -1:, :] - inside_block)
    block_states = jnp.einsum(
        "sblhn,sblhp->sbhpn", key_heads, x_blocks * tail_weight[..., None], precision=PRECISE
    )
    block_totals = inside_block[:, :, -1, :]
    running = jnp.zeros((seq_count, heads_here, HEAD_DIM, STATE), jnp.float32)
    entering = [running]
    running = jnp.exp(block_totals[:, 0])[:, :, None, None] * running + block_states[:, 0]
    entering_states = jnp.stack(entering, axis=1)
    forwarded_portion = jnp.einsum(
        "sblhn,sbhpn->sblhp", query_heads, entering_states, precision=PRECISE
    )
    forwarded_portion = forwarded_portion * jnp.exp(inside_block)[..., None]
    local_out = (inner_part + forwarded_portion).reshape(seq_count, seg_len, heads_here, HEAD_DIM)
    decay_total = jnp.exp(jnp.sum(block_totals, axis=1))
    prefix_log = jnp.cumsum(log_decay, axis=1)
    return (local_out, decay_total, running, prefix_log)


def read_in(local_out, readout_vectors, prefix_log, incoming):
    query_heads = jnp.repeat(readout_vectors, HEAD_TOTAL // GROUPS, axis=2)
    carried = jnp.einsum("slhn,shpn->slhp", query_heads, incoming, precision=PRECISE)
    return local_out + carried * jnp.exp(prefix_log)[..., None]


def combine(preceding_portion, latter):
    return (
        preceding_portion[0] * latter[0],
        latter[0][:, :, None, None] * preceding_portion[1] + latter[1],
    )


def body(
    tokens,
    in_gain,
    gate_weight,
    input_weight,
    key_weight,
    query_weight,
    step_weight,
    conv_input,
    conv_key,
    conv_query,
    step_bias,
    decay_rate,
    decay_extra,
    out_gain,
    out_weight,
):
    normed = rms_rows(tokens.astype(jnp.float32), in_gain).astype(jnp.bfloat16)
    joined_weight = jnp.concatenate(
        [gate_weight, input_weight, key_weight, query_weight, step_weight], axis=1
    )
    token_segment = lax.all_gather(normed, "tp", axis=1, tiled=True)
    seq_count = token_segment.shape[0]
    row_count = token_segment.shape[1]
    result = jnp.dot(
        token_segment.reshape(seq_count * row_count, token_segment.shape[2]),
        joined_weight,
        preferred_element_type=jnp.float32,
    )
    projected = result.astype(jnp.bfloat16).reshape(seq_count, row_count, joined_weight.shape[1])
    seq_count, seg_len = (projected.shape[0], projected.shape[1])
    inner_here = gate_weight.shape[1]
    state_cols = key_weight.shape[1]
    heads_here = step_bias.shape[0]
    gate_in = projected[:, :, :inner_here]
    conv_in = projected[:, :, inner_here : 2 * inner_here + 2 * state_cols]
    step_all = projected[:, :, 2 * inner_here + 2 * state_cols :]
    rim_rows = from_behind(conv_in[:, seg_len - CONV + 1 :, :], "sp", 1)
    conv_weights = jnp.concatenate([conv_input, conv_key, conv_query], axis=1)
    conv_out = causal_blend(rim_rows, conv_in, conv_weights)
    conv_values = conv_out[:, :, :inner_here].reshape(seq_count, seg_len, heads_here, HEAD_DIM)
    keys_b = conv_out[:, :, inner_here : inner_here + state_cols].reshape(
        seq_count, seg_len, state_cols // STATE, STATE
    )
    readout_vectors = conv_out[:, :, inner_here + state_cols :].reshape(
        seq_count, seg_len, state_cols // STATE, STATE
    )
    own_steps = lax.dynamic_slice_in_dim(step_all, lax.axis_index("tp") * heads_here, heads_here, 2)
    step_size = jax.nn.softplus(own_steps.astype(jnp.float32) + step_bias)
    log_decay = -step_size * decay_rate + jnp.transpose(decay_extra, (0, 2, 1))
    scaled_x = conv_values * step_size[..., None]
    local_out, decay_total, final_state, prefix_log = local_pass(
        scaled_x, keys_b, readout_vectors, log_decay
    )
    incoming = carried_in(
        (decay_total, final_state),
        "sp",
        combine,
        (jnp.ones_like(decay_total), jnp.zeros_like(final_state)),
    )
    blended_heads = read_in(local_out, readout_vectors, prefix_log, incoming[1])
    gated_rows = blended_heads.reshape(seq_count, seg_len, inner_here) * jax.nn.silu(
        gate_in.astype(jnp.float32)
    )
    group_width = HEAD_TOTAL // GROUPS * HEAD_DIM
    groups_here = inner_here // group_width
    normed_out = rms_rows(
        gated_rows.reshape(seq_count, seg_len, groups_here, group_width),
        out_gain.reshape(groups_here, group_width),
    )
    normed_out = normed_out.reshape(seq_count, seg_len, inner_here).astype(jnp.bfloat16)
    token_rows = lax.all_to_all(normed_out, "tp", split_axis=1, concat_axis=2, tiled=True)
    result = jnp.dot(
        token_rows.reshape(token_rows.shape[0] * token_rows.shape[1], token_rows.shape[2]),
        out_weight,
        preferred_element_type=jnp.float32,
    )
    return result.astype(jnp.bfloat16).reshape(
        token_rows.shape[0], token_rows.shape[1], out_weight.shape[1]
    )

MESH = pl.DeviceIdType.MESH


def fused_kernel(
    dims,
    tok, gain, gw, iw, kw, qw, sw, cx, ck, cq, sb, dr, de, og, ow,
    out,
    W, SW, OW, tokg, pay, aux, payr, auxr, mix, fin,
    wsem, own_sem, xs, xr, ps, pr, fs, fr, ds, dsa, rs, rsa, ms, mr,
):
    nsp, ntp, S, R, D, inner, st, heads = dims
    bf, f32 = jnp.bfloat16, jnp.float32
    width = HEAD_TOTAL // GROUPS * HEAD_DIM
    G = inner // width
    X = ntp // 2
    N = ntp * R
    ratio = HEAD_TOTAL // GROUPS
    sp = lax.axis_index("sp")
    tp = lax.axis_index("tp")
    x, c = tp // 2, tp % 2
    partner = x * 2 + 1 - c
    me = sp * ntp + tp
    total = nsp * ntp

    parts = [
        (gw, W.at[:, 0:inner]),
        (iw, W.at[:, inner : 2 * inner]),
        (kw, W.at[:, 2 * inner : 2 * inner + st]),
        (qw, W.at[:, 2 * inner + st : 2 * inner + 2 * st]),
        (sw, SW),
        (ow, OW),
    ]
    loads = [pltpu.make_async_copy(a, b, wsem.at[i]) for i, (a, b) in enumerate(parts)]
    for load in loads[:5]:
        load.start()
    own = pltpu.make_async_copy(tok, tokg.at[:, tp], own_sem)
    own.start()

    barrier = pltpu.get_barrier_semaphore()

    def greet(d, carry):
        other = (me + d) % total
        pl.semaphore_signal(
            barrier, inc=1, device_id=(other // ntp, other % ntp), device_id_type=MESH
        )
        return carry

    lax.fori_loop(1, total, greet, 0)
    pl.semaphore_wait(barrier, total - 1)

    def seq_of(k):
        return (sp // G + 1 + k) % S

    def cross(k, dx):
        s = seq_of(k)
        return pltpu.make_async_remote_copy(
            src_ref=tok.at[s], dst_ref=tokg.at[s, tp],
            send_sem=xs.at[dx - 1, k], recv_sem=xr.at[dx - 1, k],
            device_id=(sp, (x + dx) % X * 2 + c), device_id_type=MESH,
        )

    def beside(k):
        s = seq_of(k)
        return pltpu.make_async_remote_copy(
            src_ref=tok.at[s], dst_ref=tokg.at[s, tp],
            send_sem=ps.at[k], recv_sem=pr.at[k],
            device_id=(sp, partner), device_id_type=MESH,
        )

    def passed_on(k, dx):
        s = seq_of(k)
        source = (x - dx + X) % X * 2 + c
        return pltpu.make_async_remote_copy(
            src_ref=tokg.at[s, source], dst_ref=tokg.at[s, source],
            send_sem=fs.at[dx - 1, k], recv_sem=fr.at[dx - 1, k],
            device_id=(sp, partner), device_id_type=MESH,
        )

    for k in range(S):
        for dx in range(1, X):
            cross(k, dx).start()
    for k in range(S):
        beside(k).start()
    loads[5].start()

    def out_pair(dest):
        args = dict(device_id=(dest, tp), device_id_type=MESH)
        return (
            pltpu.make_async_remote_copy(
                src_ref=pay.at[dest], dst_ref=payr.at[sp],
                send_sem=ds.at[dest], recv_sem=rs.at[sp], **args,
            ),
            pltpu.make_async_remote_copy(
                src_ref=aux.at[dest], dst_ref=auxr.at[sp],
                send_sem=dsa.at[dest], recv_sem=rsa.at[sp], **args,
            ),
        )

    def project(k):
        s = seq_of(k)
        t = tokg[s].reshape(N, D).astype(f32)
        scale = lax.rsqrt(jnp.mean(t * t, axis=-1, keepdims=True) + NORM_EPS)
        n = (t * scale * gain[...]).astype(bf)
        p = jnp.dot(n, W[...], preferred_element_type=f32)
        steps = jnp.dot(n, SW[...], preferred_element_type=f32).astype(bf).astype(f32)
        steps = steps.T
        mine = steps[0:heads]
        for j in range(1, ntp):
            mine = jnp.where(tp == j, steps[j * heads : (j + 1) * heads], mine)
        dt = jax.nn.softplus(mine + sb[...])
        ld = de[s] - dt * dr[...]
        for g in range(G):
            dest = s * G + g
            keys = p[:, 2 * inner + g * STATE : 2 * inner + (g + 1) * STATE]
            queries = p[:, 2 * inner + st + g * STATE : 2 * inner + st + (g + 1) * STATE]
            pay[dest, :, 0:width] = p[:, inner + g * width : inner + (g + 1) * width].astype(bf)
            pay[dest, :, width : width + 2 * STATE] = jnp.concatenate(
                [keys, queries], axis=1
            ).astype(bf)
            pay[dest, :, width + 2 * STATE :] = p[:, g * width : (g + 1) * width].astype(bf)
            rows = jnp.concatenate(
                [
                    dt[g * ratio : (g + 1) * ratio],
                    ld[g * ratio : (g + 1) * ratio],
                    jnp.zeros((8 - 2 * ratio, N), f32),
                ],
                axis=0,
            )
            aux[dest] = jnp.concatenate([rows, jnp.zeros((8, 128 - N), f32)], axis=1)

            @pl.when(dest != sp)
            def _():
                for copy in out_pair(dest):
                    copy.start()

            @pl.when(dest == sp)
            def _():
                pltpu.make_async_copy(pay.at[dest], payr.at[sp], rs.at[sp]).start()
                pltpu.make_async_copy(aux.at[dest], auxr.at[sp], rsa.at[sp]).start()

    for load in loads[:5]:
        load.wait()
    own.wait()
    for k in range(S + 1):
        if k < S:
            for dx in range(1, X):
                cross(k, dx).wait_recv()
                passed_on(k, dx).start()
        if k >= 1:
            beside(k - 1).wait_recv()
            for dx in range(1, X):
                passed_on(k - 1, dx).wait_recv()
            project(k - 1)

    g = sp % G
    mine_seq = sp // G
    L = nsp * N

    def pick(make):
        chosen = make(0)
        for j in range(1, G):
            chosen = jnp.where(g == j, make(j), chosen)
        return chosen

    taps = pick(
        lambda j: jnp.concatenate(
            [
                cx[:, j * width : (j + 1) * width],
                ck[:, j * STATE : (j + 1) * STATE],
                cq[:, j * STATE : (j + 1) * STATE],
            ],
            axis=1,
        )
    )
    gain_out = pick(lambda j: og[:, j * width : (j + 1) * width])

    for b in range(nsp):
        pltpu.make_async_copy(payr.at[b], payr.at[b], rs.at[b]).wait()
        pltpu.make_async_copy(auxr.at[b], auxr.at[b], rsa.at[b]).wait()

    A = auxr[...].reshape(nsp * 8, 128)
    upto = lax.broadcasted_iota(jnp.int32, (128, 128), 0) <= lax.broadcasted_iota(
        jnp.int32, (128, 128), 1
    )
    cum = jnp.dot(A, upto.astype(f32), precision=PRECISE, preferred_element_type=f32)
    AT, cumT = A.T, cum.T
    conv_w = width + 2 * STATE
    first_head = lax.broadcasted_iota(jnp.int32, (N, width), 1) < HEAD_DIM
    first_row = lax.broadcasted_iota(jnp.int32, (1, width), 1) < HEAD_DIM
    causal = lax.broadcasted_iota(jnp.int32, (N, N), 0) >= lax.broadcasted_iota(
        jnp.int32, (N, N), 1
    )
    row_id = lax.broadcasted_iota(jnp.int32, (N, conv_w), 0)
    channel = tp * G + g

    def result_copy(b, j):
        return pltpu.make_async_remote_copy(
            src_ref=mix.at[b, j],
            dst_ref=fin.at[mine_seq, :, pl.ds(pl.multiple_of(channel * width, width), width)],
            send_sem=ms.at[b * ntp + j], recv_sem=mr.at[me],
            device_id=(b, j), device_id_type=MESH,
        )

    state = jnp.zeros((STATE, width), f32)
    before = jnp.zeros((N, conv_w), f32)
    for b in range(nsp):
        now = payr[b, :, 0:conv_w].astype(f32)
        acc = now * taps[CONV - 1 : CONV]
        for k in range(1, CONV):
            shifted = jnp.where(row_id < k, pltpu.roll(before, k, 0), pltpu.roll(now, k, 0))
            acc = acc + shifted * taps[CONV - 1 - k : CONV - k]
        before = now
        v = jax.nn.silu(acc)
        kb = v[:, width : width + STATE].astype(bf)
        qb = v[:, width + STATE :].astype(bf)
        r = b * 8
        cols = [cumT[0:N, r + ratio + h : r + ratio + h + 1] for h in range(2)]
        rows = [cum[r + ratio + h : r + ratio + h + 1, 0:N] for h in range(2)]
        tots = [cum[r + ratio + h : r + ratio + h + 1, 127:128] for h in range(2)]
        step = jnp.where(first_head, AT[0:N, r : r + 1], AT[0:N, r + 1 : r + 2])
        reach = jnp.where(first_head, cols[0], cols[1])
        total_row = jnp.where(first_row, tots[0], tots[1])
        xd = v[:, 0:width] * step
        xb = xd.astype(bf)
        scores = lax.dot_general(qb, kb, (((1,), (1,)), ((), ())), preferred_element_type=f32)
        inner_parts = []
        for h in range(2):
            spread = jnp.where(causal, cols[h] - rows[h], 0.0)
            weights = jnp.where(causal, scores * jnp.exp(spread), 0.0).astype(bf)
            inner_parts.append(jnp.dot(weights, xb, preferred_element_type=f32))
        y = jnp.where(first_head, inner_parts[0], inner_parts[1])
        y = y + jnp.dot(qb, state.astype(bf), preferred_element_type=f32) * jnp.exp(reach)
        tail = (xd * jnp.exp(total_row - reach)).astype(bf)
        fresh = lax.dot_general(kb, tail, (((0,), (0,)), ((), ())), preferred_element_type=f32)
        state = jnp.exp(total_row) * state + fresh
        gated = y * jax.nn.silu(payr[b, :, conv_w:].astype(f32))
        scale = lax.rsqrt(jnp.mean(gated * gated, axis=-1, keepdims=True) + NORM_EPS)
        mix[b] = (gated * scale * gain_out).astype(bf).reshape(ntp, R, width)
        for j in range(ntp):
            same = jnp.logical_and(sp == b, tp == j)

            @pl.when(jnp.logical_not(same))
            def _():
                result_copy(b, j).start()

            @pl.when(same)
            def _():
                pltpu.make_async_copy(
                    mix.at[b, j],
                    fin.at[mine_seq, :, pl.ds(pl.multiple_of(channel * width, width), width)],
                    mr.at[me],
                ).start()

    loads[5].wait()
    for i in range(total):
        slot = fin.at[i // ntp // G, :, pl.ds((i % ntp * G + i // ntp % G) * width, width)]
        pltpu.make_async_copy(slot, slot, mr.at[i]).wait()
    rows = fin[...].reshape(S * R, ntp * inner)
    res = jnp.dot(rows, OW[...], preferred_element_type=f32)
    out[...] = res.astype(bf).reshape(S, R, D)

    for k in range(S):
        for dx in range(1, X):
            cross(k, dx).wait_send()
            passed_on(k, dx).wait_send()
        beside(k).wait_send()
    for b in range(nsp):

        @pl.when(b != sp)
        def _():
            for copy in out_pair(b):
                copy.wait_send()

        for j in range(ntp):

            @pl.when(jnp.logical_not(jnp.logical_and(sp == b, tp == j)))
            def _():
                result_copy(b, j).wait_send()


def fused_body(
    nsp, ntp,
    tokens, in_gain, gate_weight, input_weight, key_weight, query_weight, step_weight,
    conv_input, conv_key, conv_query, step_bias, decay_rate, decay_extra, out_gain, out_weight,
):
    S, R, D = tokens.shape
    inner, st, heads = gate_weight.shape[1], key_weight.shape[1], step_bias.shape[0]
    dims = (nsp, ntp, S, R, D, inner, st, heads)
    width = HEAD_TOTAL // GROUPS * HEAD_DIM
    N, X = ntp * R, ntp // 2
    pay_w = 2 * width + 2 * STATE
    bf, f32 = jnp.bfloat16, jnp.float32
    dma = pltpu.SemaphoreType.DMA
    vmem = pl.BlockSpec(memory_space=pltpu.VMEM)
    hbm = pl.BlockSpec(memory_space=pl.ANY)
    return pl.pallas_call(
        functools.partial(fused_kernel, dims),
        out_shape=jax.ShapeDtypeStruct((S, R, out_weight.shape[1]), bf),
        in_specs=[vmem, vmem, hbm, hbm, hbm, hbm, hbm] + [vmem] * 7 + [hbm],
        out_specs=vmem,
        scratch_shapes=[
            pltpu.VMEM((D, 2 * inner + 2 * st), bf),
            pltpu.VMEM(step_weight.shape, bf),
            pltpu.VMEM(out_weight.shape, bf),
            pltpu.VMEM((S, ntp, R, D), bf),
            pltpu.VMEM((nsp, N, pay_w), bf),
            pltpu.VMEM((nsp, 8, 128), f32),
            pltpu.VMEM((nsp, N, pay_w), bf),
            pltpu.VMEM((nsp, 8, 128), f32),
            pltpu.VMEM((nsp, ntp, R, width), bf),
            pltpu.VMEM((S, R, ntp * inner), bf),
            dma((6,)),
            dma,
            dma((X - 1, S)), dma((X - 1, S)),
            dma((S,)), dma((S,)),
            dma((X - 1, S)), dma((X - 1, S)),
            dma((nsp,)), dma((nsp,)), dma((nsp,)), dma((nsp,)),
            dma((nsp * ntp,)), dma((nsp * ntp,)),
        ],
        compiler_params=pltpu.CompilerParams(
            collective_id=0, has_side_effects=True, vmem_limit_bytes=56 * 1024 * 1024
        ),
        name="mixer",
    )(
        tokens, in_gain.reshape(1, -1), gate_weight, input_weight, key_weight, query_weight,
        step_weight, conv_input, conv_key, conv_query, step_bias.reshape(-1, 1),
        decay_rate.reshape(-1, 1), decay_extra, out_gain.reshape(1, -1), out_weight,
    )


def fits(nsp, ntp, tokens, inner, st, length):
    seqs = tokens[0]
    width = HEAD_TOTAL // GROUPS * HEAD_DIM
    rows = length // (nsp * ntp)
    return (
        ntp % 2 == 0 and ntp > 2 and inner % width == 0 and width == 128
        and 2 * STATE == 128 and HEAD_TOTAL // GROUPS == 2
        and seqs * (inner // width) == nsp and rows % 16 == 0 and rows * ntp == BLOCK
    )


def solution(mesh):
    placed = (
        P(None, ("sp", "tp"), None),
        P(),
        P(None, "tp"),
        P(None, "tp"),
        P(None, "tp"),
        P(None, "tp"),
        P(),
        P(None, "tp"),
        P(None, "tp"),
        P(None, "tp"),
        P("tp"),
        P("tp"),
        P(None, "tp", "sp"),
        P("tp"),
        P(),
    )
    nsp, ntp = mesh.shape["sp"], mesh.shape["tp"]

    def chosen(*args):
        inner, st = args[2].shape[1], args[4].shape[1]
        rows = args[0].shape[1] * nsp * ntp
        if fits(nsp, ntp, args[0].shape, inner, st, rows):
            return fused_body(nsp, ntp, *args)
        return body(*args)

    return jax.shard_map(
        chosen, mesh=mesh, in_specs=placed, out_specs=P(None, ("sp", "tp"), None), check_vma=False
    )
```

```python
import functools

import jax
import jax.numpy as jnp
from jax import lax
from jax.experimental import pallas as pl
from jax.experimental.pallas import tpu as pltpu
from jax.sharding import PartitionSpec as P

HEAD_TOTAL = 16
HEAD_DIM = 64
GROUPS = 8
STATE = 64
CONV = 4
BLOCK = 64


NORM_EPS = 1e-06
PRECISE = lax.Precision.HIGHEST


def from_behind(array, axis, by):
    length = lax.axis_size(axis)
    pairs = [(i, i + by) for i in range(length) if 0 <= i + by < length]
    return lax.ppermute(array, axis, pairs)


def carried_in(array, axis, combine, identity):
    length, place = (lax.axis_size(axis), lax.axis_index(axis))
    everything = jax.tree.map(lambda part: lax.all_gather(part, axis), array)
    start = jax.tree.map(
        lambda part, zero: jnp.broadcast_to(jnp.asarray(zero, part.dtype), part.shape),
        array,
        identity,
    )

    def step(k, before):
        reached = k < place
        new = combine(before, jax.tree.map(lambda part: part[k], everything))
        return jax.tree.map(lambda a, b: jnp.where(reached, a, b), new, before)

    return lax.fori_loop(0, length, step, start)


def rms_rows(values, gain_row):
    mean_sq = jnp.mean(values * values, axis=-1, keepdims=True)
    return values * lax.rsqrt(mean_sq + NORM_EPS) * gain_row


def causal_blend(rim_rows, local_rows, weights):
    length = local_rows.shape[1]
    padded = jnp.concatenate([rim_rows, local_rows], axis=1).astype(jnp.float32)
    summed_rows = padded[:, 0:length, :] * weights[0]
    for offset in range(1, weights.shape[0]):
        summed_rows = summed_rows + padded[:, offset : offset + length, :] * weights[offset]
    return jax.nn.silu(summed_rows)


def local_pass(scaled_x, keys_b, readout_vectors, log_decay):
    seq_count, seg_len, heads_here = (scaled_x.shape[0], scaled_x.shape[1], scaled_x.shape[2])
    blocks_here = seg_len // BLOCK
    ratio_heads = HEAD_TOTAL // GROUPS

    def to_blocks(tensor):
        return tensor.reshape((seq_count, blocks_here, BLOCK) + tensor.shape[2:])

    x_blocks = to_blocks(scaled_x)
    b_blocks = to_blocks(keys_b)
    c_blocks = to_blocks(readout_vectors)
    inside_block = jnp.cumsum(to_blocks(log_decay), axis=2)
    causal = jnp.tril(jnp.ones((BLOCK, BLOCK), bool))[None, None, :, :, None]
    spread_log = inside_block[:, :, :, None, :] - inside_block[:, :, None, :, :]
    decay_matrix = jnp.where(causal, jnp.exp(jnp.where(causal, spread_log, 0.0)), 0.0)
    scores = jnp.einsum("sblgn,sbtgn->sbltg", c_blocks, b_blocks, precision=PRECISE)
    scores = jnp.repeat(scores, ratio_heads, axis=4)
    key_heads = jnp.repeat(b_blocks, ratio_heads, axis=3)
    query_heads = jnp.repeat(c_blocks, ratio_heads, axis=3)
    inner_part = jnp.einsum(
        "sblth,sbthp->sblhp", scores * decay_matrix, x_blocks, precision=PRECISE
    )
    tail_weight = jnp.exp(inside_block[:, :, -1:, :] - inside_block)
    block_states = jnp.einsum(
        "sblhn,sblhp->sbhpn", key_heads, x_blocks * tail_weight[..., None], precision=PRECISE
    )
    block_totals = inside_block[:, :, -1, :]
    running = jnp.zeros((seq_count, heads_here, HEAD_DIM, STATE), jnp.float32)
    entering = [running]
    running = jnp.exp(block_totals[:, 0])[:, :, None, None] * running + block_states[:, 0]
    entering_states = jnp.stack(entering, axis=1)
    forwarded_portion = jnp.einsum(
        "sblhn,sbhpn->sblhp", query_heads, entering_states, precision=PRECISE
    )
    forwarded_portion = forwarded_portion * jnp.exp(inside_block)[..., None]
    local_out = (inner_part + forwarded_portion).reshape(seq_count, seg_len, heads_here, HEAD_DIM)
    decay_total = jnp.exp(jnp.sum(block_totals, axis=1))
    prefix_log = jnp.cumsum(log_decay, axis=1)
    return (local_out, decay_total, running, prefix_log)


def read_in(local_out, readout_vectors, prefix_log, incoming):
    query_heads = jnp.repeat(readout_vectors, HEAD_TOTAL // GROUPS, axis=2)
    carried = jnp.einsum("slhn,shpn->slhp", query_heads, incoming, precision=PRECISE)
    return local_out + carried * jnp.exp(prefix_log)[..., None]


def combine(preceding_portion, latter):
    return (
        preceding_portion[0] * latter[0],
        latter[0][:, :, None, None] * preceding_portion[1] + latter[1],
    )


def body(
    tokens,
    in_gain,
    gate_weight,
    input_weight,
    key_weight,
    query_weight,
    step_weight,
    conv_input,
    conv_key,
    conv_query,
    step_bias,
    decay_rate,
    decay_extra,
    out_gain,
    out_weight,
):
    normed = rms_rows(tokens.astype(jnp.float32), in_gain).astype(jnp.bfloat16)
    joined_weight = jnp.concatenate(
        [gate_weight, input_weight, key_weight, query_weight, step_weight], axis=1
    )
    token_segment = lax.all_gather(normed, "tp", axis=1, tiled=True)
    seq_count = token_segment.shape[0]
    row_count = token_segment.shape[1]
    result = jnp.dot(
        token_segment.reshape(seq_count * row_count, token_segment.shape[2]),
        joined_weight,
        preferred_element_type=jnp.float32,
    )
    projected = result.astype(jnp.bfloat16).reshape(seq_count, row_count, joined_weight.shape[1])
    seq_count, seg_len = (projected.shape[0], projected.shape[1])
    inner_here = gate_weight.shape[1]
    state_cols = key_weight.shape[1]
    heads_here = step_bias.shape[0]
    gate_in = projected[:, :, :inner_here]
    conv_in = projected[:, :, inner_here : 2 * inner_here + 2 * state_cols]
    step_all = projected[:, :, 2 * inner_here + 2 * state_cols :]
    rim_rows = from_behind(conv_in[:, seg_len - CONV + 1 :, :], "sp", 1)
    conv_weights = jnp.concatenate([conv_input, conv_key, conv_query], axis=1)
    conv_out = causal_blend(rim_rows, conv_in, conv_weights)
    conv_values = conv_out[:, :, :inner_here].reshape(seq_count, seg_len, heads_here, HEAD_DIM)
    keys_b = conv_out[:, :, inner_here : inner_here + state_cols].reshape(
        seq_count, seg_len, state_cols // STATE, STATE
    )
    readout_vectors = conv_out[:, :, inner_here + state_cols :].reshape(
        seq_count, seg_len, state_cols // STATE, STATE
    )
    own_steps = lax.dynamic_slice_in_dim(step_all, lax.axis_index("tp") * heads_here, heads_here, 2)
    step_size = jax.nn.softplus(own_steps.astype(jnp.float32) + step_bias)
    log_decay = -step_size * decay_rate + jnp.transpose(decay_extra, (0, 2, 1))
    scaled_x = conv_values * step_size[..., None]
    local_out, decay_total, final_state, prefix_log = local_pass(
        scaled_x, keys_b, readout_vectors, log_decay
    )
    incoming = carried_in(
        (decay_total, final_state),
        "sp",
        combine,
        (jnp.ones_like(decay_total), jnp.zeros_like(final_state)),
    )
    blended_heads = read_in(local_out, readout_vectors, prefix_log, incoming[1])
    gated_rows = blended_heads.reshape(seq_count, seg_len, inner_here) * jax.nn.silu(
        gate_in.astype(jnp.float32)
    )
    group_width = HEAD_TOTAL // GROUPS * HEAD_DIM
    groups_here = inner_here // group_width
    normed_out = rms_rows(
        gated_rows.reshape(seq_count, seg_len, groups_here, group_width),
        out_gain.reshape(groups_here, group_width),
    )
    normed_out = normed_out.reshape(seq_count, seg_len, inner_here).astype(jnp.bfloat16)
    token_rows = lax.all_to_all(normed_out, "tp", split_axis=1, concat_axis=2, tiled=True)
    result = jnp.dot(
        token_rows.reshape(token_rows.shape[0] * token_rows.shape[1], token_rows.shape[2]),
        out_weight,
        preferred_element_type=jnp.float32,
    )
    return result.astype(jnp.bfloat16).reshape(
        token_rows.shape[0], token_rows.shape[1], out_weight.shape[1]
    )

MESH = pl.DeviceIdType.MESH


def fused_kernel(
    dims,
    tok, gain, gw, iw, kw, qw, sw, cx, ck, cq, sb, dr, de, og, ow,
    out,
    W, SW, OW, tokg, pay, aux, payr, auxr, mix, fin,
    wsem, own_sem, xs, xr, ps, pr, fs, fr, ds, dsa, rs, rsa, ms, mr, round_sem,
):
    nsp, ntp, S, R, D, inner, st, heads = dims
    bf, f32 = jnp.bfloat16, jnp.float32
    width = HEAD_TOTAL // GROUPS * HEAD_DIM
    G = inner // width
    X = ntp // 2
    N = ntp * R
    ratio = HEAD_TOTAL // GROUPS
    sp = lax.axis_index("sp")
    tp = lax.axis_index("tp")
    x, c = tp // 2, tp % 2
    partner = x * 2 + 1 - c
    me = sp * ntp + tp
    total = nsp * ntp

    parts = [
        (gw, W.at[:, 0:inner]),
        (iw, W.at[:, inner : 2 * inner]),
        (kw, W.at[:, 2 * inner : 2 * inner + st]),
        (qw, W.at[:, 2 * inner + st : 2 * inner + 2 * st]),
        (sw, SW),
        (ow, OW),
    ]
    loads = [pltpu.make_async_copy(a, b, wsem.at[i]) for i, (a, b) in enumerate(parts)]
    for load in loads[:5]:
        load.start()
    own = pltpu.make_async_copy(tok, tokg.at[:, tp], own_sem)
    own.start()

    barrier = pltpu.get_barrier_semaphore()

    def near(sem):
        row = sp // G
        for d in range(1, G):
            other = row * G + (sp + d) % G
            pl.semaphore_signal(sem, inc=1, device_id=(other, tp), device_id_type=MESH)

        @pl.when(row > 0)
        def _():
            pl.semaphore_signal(sem, inc=1, device_id=(sp - G, tp), device_id_type=MESH)

        @pl.when(row < S - 1)
        def _():
            pl.semaphore_signal(sem, inc=1, device_id=(sp + G, tp), device_id_type=MESH)

    def near_wait(sem, extra):
        row = sp // G
        ends = jnp.where(row > 0, 1, 0) + jnp.where(row < S - 1, 1, 0)
        pl.semaphore_wait(sem, G - 1 + extra + ends)

    for d in range(1, ntp):
        pl.semaphore_signal(
            barrier, inc=1, device_id=(sp, (tp + d) % ntp), device_id_type=MESH
        )
    near(barrier)
    near_wait(barrier, ntp - 1)

    def seq_of(k):
        return (sp // G + 1 + k) % S

    def cross(k, dx):
        s = seq_of(k)
        return pltpu.make_async_remote_copy(
            src_ref=tok.at[s], dst_ref=tokg.at[s, tp],
            send_sem=xs.at[dx - 1, k], recv_sem=xr.at[dx - 1, k],
            device_id=(sp, (x + dx) % X * 2 + c), device_id_type=MESH,
        )

    def beside(k):
        s = seq_of(k)
        return pltpu.make_async_remote_copy(
            src_ref=tok.at[s], dst_ref=tokg.at[s, tp],
            send_sem=ps.at[k], recv_sem=pr.at[k],
            device_id=(sp, partner), device_id_type=MESH,
        )

    def passed_on(k, dx):
        s = seq_of(k)
        source = (x - dx + X) % X * 2 + c
        return pltpu.make_async_remote_copy(
            src_ref=tokg.at[s, source], dst_ref=tokg.at[s, source],
            send_sem=fs.at[dx - 1, k], recv_sem=fr.at[dx - 1, k],
            device_id=(sp, partner), device_id_type=MESH,
        )

    for k in range(S):
        for dx in range(1, X):
            cross(k, dx).start()
    for k in range(S):
        beside(k).start()
    loads[5].start()
    for i in range(S - 1):
        near(round_sem.at[i])
        near_wait(round_sem.at[i], 0)

    def out_pair(dest):
        args = dict(device_id=(dest, tp), device_id_type=MESH)
        return (
            pltpu.make_async_remote_copy(
                src_ref=pay.at[dest], dst_ref=payr.at[sp],
                send_sem=ds.at[dest], recv_sem=rs.at[sp], **args,
            ),
            pltpu.make_async_remote_copy(
                src_ref=aux.at[dest], dst_ref=auxr.at[sp],
                send_sem=dsa.at[dest], recv_sem=rsa.at[sp], **args,
            ),
        )

    head_id = lax.broadcasted_iota(jnp.int32, (heads, N), 0)
    bias_col = jnp.zeros((heads, N), f32)
    rate_col = jnp.zeros((heads, N), f32)
    for h in range(heads):
        bias_col = jnp.where(head_id == h, sb[h], bias_col)
        rate_col = jnp.where(head_id == h, dr[h], rate_col)

    def project(k):
        s = seq_of(k)
        t = tokg[s].reshape(N, D).astype(f32)
        scale = lax.rsqrt(jnp.mean(t * t, axis=-1, keepdims=True) + NORM_EPS)
        n = (t * scale * gain[...]).astype(bf)
        p = jnp.dot(n, W[...], preferred_element_type=f32)
        steps = lax.dot_general(
            SW[...], n, (((1,), (1,)), ((), ())), preferred_element_type=f32
        )
        steps = steps.astype(bf).astype(f32)
        mine = steps[0:heads]
        for j in range(1, ntp):
            mine = jnp.where(tp == j, steps[j * heads : (j + 1) * heads], mine)
        dt = jax.nn.softplus(mine + bias_col)
        ld = de[s] - dt * rate_col
        for g in range(G):
            dest = s * G + g
            keys = p[:, 2 * inner + g * STATE : 2 * inner + (g + 1) * STATE]
            queries = p[:, 2 * inner + st + g * STATE : 2 * inner + st + (g + 1) * STATE]
            pay[dest, :, 0:width] = p[:, inner + g * width : inner + (g + 1) * width].astype(bf)
            pay[dest, :, width : width + 2 * STATE] = jnp.concatenate(
                [keys, queries], axis=1
            ).astype(bf)
            pay[dest, :, width + 2 * STATE :] = p[:, g * width : (g + 1) * width].astype(bf)
            rows = jnp.concatenate(
                [
                    dt[g * ratio : (g + 1) * ratio],
                    ld[g * ratio : (g + 1) * ratio],
                    jnp.zeros((8 - 2 * ratio, N), f32),
                ],
                axis=0,
            )
            aux[dest] = jnp.concatenate([rows, jnp.zeros((8, 128 - N), f32)], axis=1)

            @pl.when(dest != sp)
            def _():
                for copy in out_pair(dest):
                    copy.start()

            @pl.when(dest == sp)
            def _():
                pltpu.make_async_copy(pay.at[dest], payr.at[sp], rs.at[sp]).start()
                pltpu.make_async_copy(aux.at[dest], auxr.at[sp], rsa.at[sp]).start()

    for load in loads[:5]:
        load.wait()
    own.wait()
    for k in range(S + 1):
        if k < S:
            for dx in range(1, X):
                cross(k, dx).wait_recv()
                passed_on(k, dx).start()
        if k >= 1:
            beside(k - 1).wait_recv()
            for dx in range(1, X):
                passed_on(k - 1, dx).wait_recv()
            project(k - 1)

    g = sp % G
    mine_seq = sp // G
    L = nsp * N

    def pick(make):
        chosen = make(0)
        for j in range(1, G):
            chosen = jnp.where(g == j, make(j), chosen)
        return chosen

    taps = pick(
        lambda j: jnp.concatenate(
            [
                cx[:, j * width : (j + 1) * width],
                ck[:, j * STATE : (j + 1) * STATE],
                cq[:, j * STATE : (j + 1) * STATE],
            ],
            axis=1,
        )
    )
    gain_out = pick(lambda j: og[:, j * width : (j + 1) * width])

    for b in range(nsp):
        pltpu.make_async_copy(payr.at[b], payr.at[b], rs.at[b]).wait()
        pltpu.make_async_copy(auxr.at[b], auxr.at[b], rsa.at[b]).wait()

    A = auxr[...].reshape(nsp * 8, 128)
    upto = lax.broadcasted_iota(jnp.int32, (128, 128), 0) <= lax.broadcasted_iota(
        jnp.int32, (128, 128), 1
    )
    cum = jnp.dot(A, upto.astype(f32), precision=PRECISE, preferred_element_type=f32)
    AT, cumT = A.T, cum.T
    conv_w = width + 2 * STATE
    first_head = lax.broadcasted_iota(jnp.int32, (N, width), 1) < HEAD_DIM
    first_row = lax.broadcasted_iota(jnp.int32, (1, width), 1) < HEAD_DIM
    causal = lax.broadcasted_iota(jnp.int32, (N, N), 0) >= lax.broadcasted_iota(
        jnp.int32, (N, N), 1
    )
    row_id = lax.broadcasted_iota(jnp.int32, (N, conv_w), 0)
    channel = tp * G + g

    def result_copy(b, j):
        return pltpu.make_async_remote_copy(
            src_ref=mix.at[b, j],
            dst_ref=fin.at[mine_seq, :, pl.ds(pl.multiple_of(channel * width, width), width)],
            send_sem=ms.at[b * ntp + j], recv_sem=mr.at[me],
            device_id=(b, j), device_id_type=MESH,
        )

    state = jnp.zeros((STATE, width), f32)
    before = jnp.zeros((N, conv_w), f32)
    for b in range(nsp):
        now = payr[b, :, 0:conv_w].astype(f32)
        acc = now * taps[CONV - 1 : CONV]
        for k in range(1, CONV):
            shifted = jnp.where(row_id < k, pltpu.roll(before, k, 0), pltpu.roll(now, k, 0))
            acc = acc + shifted * taps[CONV - 1 - k : CONV - k]
        before = now
        v = jax.nn.silu(acc)
        kb = v[:, width : width + STATE].astype(bf)
        qb = v[:, width + STATE :].astype(bf)
        r = b * 8
        cols = [cumT[0:N, r + ratio + h : r + ratio + h + 1] for h in range(2)]
        rows = [cum[r + ratio + h : r + ratio + h + 1, 0:N] for h in range(2)]
        tots = [cum[r + ratio + h : r + ratio + h + 1, 127:128] for h in range(2)]
        step = jnp.where(first_head, AT[0:N, r : r + 1], AT[0:N, r + 1 : r + 2])
        reach = jnp.where(first_head, cols[0], cols[1])
        total_row = jnp.where(first_row, tots[0], tots[1])
        xd = v[:, 0:width] * step
        xb = xd.astype(bf)
        scores = lax.dot_general(qb, kb, (((1,), (1,)), ((), ())), preferred_element_type=f32)
        inner_parts = []
        for h in range(2):
            spread = jnp.where(causal, cols[h] - rows[h], 0.0)
            weights = jnp.where(causal, scores * jnp.exp(spread), 0.0).astype(bf)
            inner_parts.append(jnp.dot(weights, xb, preferred_element_type=f32))
        y = jnp.where(first_head, inner_parts[0], inner_parts[1])
        y = y + jnp.dot(qb, state.astype(bf), preferred_element_type=f32) * jnp.exp(reach)
        tail = (xd * jnp.exp(total_row - reach)).astype(bf)
        fresh = lax.dot_general(kb, tail, (((0,), (0,)), ((), ())), preferred_element_type=f32)
        state = jnp.exp(total_row) * state + fresh
        gated = y * jax.nn.silu(payr[b, :, conv_w:].astype(f32))
        scale = lax.rsqrt(jnp.mean(gated * gated, axis=-1, keepdims=True) + NORM_EPS)
        mix[b] = (gated * scale * gain_out).astype(bf).reshape(ntp, R, width)
        for j in range(ntp):
            same = jnp.logical_and(sp == b, tp == j)

            @pl.when(jnp.logical_not(same))
            def _():
                result_copy(b, j).start()

            @pl.when(same)
            def _():
                pltpu.make_async_copy(
                    mix.at[b, j],
                    fin.at[mine_seq, :, pl.ds(pl.multiple_of(channel * width, width), width)],
                    mr.at[me],
                ).start()

    loads[5].wait()
    for i in range(total):
        slot = fin.at[i // ntp // G, :, pl.ds((i % ntp * G + i // ntp % G) * width, width)]
        pltpu.make_async_copy(slot, slot, mr.at[i]).wait()
    rows = fin[...].reshape(S * R, ntp * inner)
    res = jnp.dot(rows, OW[...], preferred_element_type=f32)
    out[...] = res.astype(bf).reshape(S, R, D)

    for k in range(S):
        for dx in range(1, X):
            cross(k, dx).wait_send()
            passed_on(k, dx).wait_send()
        beside(k).wait_send()
    for b in range(nsp):

        @pl.when(b != sp)
        def _():
            for copy in out_pair(b):
                copy.wait_send()

        for j in range(ntp):

            @pl.when(jnp.logical_not(jnp.logical_and(sp == b, tp == j)))
            def _():
                result_copy(b, j).wait_send()


def fused_body(
    nsp, ntp,
    tokens, in_gain, gate_weight, input_weight, key_weight, query_weight, step_weight,
    conv_input, conv_key, conv_query, step_bias, decay_rate, decay_extra, out_gain, out_weight,
):
    S, R, D = tokens.shape
    inner, st, heads = gate_weight.shape[1], key_weight.shape[1], step_bias.shape[0]
    dims = (nsp, ntp, S, R, D, inner, st, heads)
    width = HEAD_TOTAL // GROUPS * HEAD_DIM
    N, X = ntp * R, ntp // 2
    pay_w = 2 * width + 2 * STATE
    bf, f32 = jnp.bfloat16, jnp.float32
    dma = pltpu.SemaphoreType.DMA
    vmem = pl.BlockSpec(memory_space=pltpu.VMEM)
    hbm = pl.BlockSpec(memory_space=pl.ANY)
    smem = pl.BlockSpec(memory_space=pltpu.SMEM)
    return pl.pallas_call(
        functools.partial(fused_kernel, dims),
        out_shape=jax.ShapeDtypeStruct((S, R, out_weight.shape[1]), bf),
        in_specs=[vmem, vmem, hbm, hbm, hbm, hbm, hbm] + [vmem] * 3 + [smem] * 2 + [vmem] * 2 + [hbm],
        out_specs=vmem,
        scratch_shapes=[
            pltpu.VMEM((D, 2 * inner + 2 * st), bf),
            pltpu.VMEM(step_weight.shape[::-1], bf),
            pltpu.VMEM(out_weight.shape, bf),
            pltpu.VMEM((S, ntp, R, D), bf),
            pltpu.VMEM((nsp, N, pay_w), bf),
            pltpu.VMEM((nsp, 8, 128), f32),
            pltpu.VMEM((nsp, N, pay_w), bf),
            pltpu.VMEM((nsp, 8, 128), f32),
            pltpu.VMEM((nsp, ntp, R, width), bf),
            pltpu.VMEM((S, R, ntp * inner), bf),
            dma((6,)),
            dma,
            dma((X - 1, S)), dma((X - 1, S)),
            dma((S,)), dma((S,)),
            dma((X - 1, S)), dma((X - 1, S)),
            dma((nsp,)), dma((nsp,)), dma((nsp,)), dma((nsp,)),
            dma((nsp * ntp,)), dma((nsp * ntp,)),
            pltpu.SemaphoreType.REGULAR((S - 1,)),
        ],
        compiler_params=pltpu.CompilerParams(
            collective_id=0, has_side_effects=True, vmem_limit_bytes=56 * 1024 * 1024
        ),
        name="mixer",
    )(
        tokens, in_gain.reshape(1, -1), gate_weight, input_weight, key_weight, query_weight,
        step_weight.T, conv_input, conv_key, conv_query, step_bias, decay_rate, decay_extra, out_gain.reshape(1, -1), out_weight,
    )


def fits(nsp, ntp, tokens, inner, st, length):
    seqs = tokens[0]
    width = HEAD_TOTAL // GROUPS * HEAD_DIM
    rows = length // (nsp * ntp)
    return (
        ntp % 2 == 0 and ntp > 2 and inner % width == 0 and width == 128
        and 2 * STATE == 128 and HEAD_TOTAL // GROUPS == 2
        and seqs * (inner // width) == nsp and rows % 16 == 0 and rows * ntp == BLOCK
    )


def solution(mesh):
    placed = (
        P(None, ("sp", "tp"), None),
        P(),
        P(None, "tp"),
        P(None, "tp"),
        P(None, "tp"),
        P(None, "tp"),
        P(),
        P(None, "tp"),
        P(None, "tp"),
        P(None, "tp"),
        P("tp"),
        P("tp"),
        P(None, "tp", "sp"),
        P("tp"),
        P(),
    )
    nsp, ntp = mesh.shape["sp"], mesh.shape["tp"]

    def chosen(*args):
        inner, st = args[2].shape[1], args[4].shape[1]
        rows = args[0].shape[1] * nsp * ntp
        if fits(nsp, ntp, args[0].shape, inner, st, rows):
            return fused_body(nsp, ntp, *args)
        return body(*args)

    return jax.shard_map(
        chosen, mesh=mesh, in_specs=placed, out_specs=P(None, ("sp", "tp"), None), check_vma=False
    )
```

```python
import functools

import jax
import jax.numpy as jnp
from jax import lax
from jax.experimental import pallas as pl
from jax.experimental.pallas import tpu as pltpu
from jax.sharding import PartitionSpec as P

HEAD_TOTAL = 16
HEAD_DIM = 64
GROUPS = 8
STATE = 64
CONV = 4
BLOCK = 64


NORM_EPS = 1e-06
PRECISE = lax.Precision.HIGHEST


def from_behind(array, axis, by):
    length = lax.axis_size(axis)
    pairs = [(i, i + by) for i in range(length) if 0 <= i + by < length]
    return lax.ppermute(array, axis, pairs)


def carried_in(array, axis, combine, identity):
    length, place = (lax.axis_size(axis), lax.axis_index(axis))
    everything = jax.tree.map(lambda part: lax.all_gather(part, axis), array)
    start = jax.tree.map(
        lambda part, zero: jnp.broadcast_to(jnp.asarray(zero, part.dtype), part.shape),
        array,
        identity,
    )

    def step(k, before):
        reached = k < place
        new = combine(before, jax.tree.map(lambda part: part[k], everything))
        return jax.tree.map(lambda a, b: jnp.where(reached, a, b), new, before)

    return lax.fori_loop(0, length, step, start)


def rms_rows(values, gain_row):
    mean_sq = jnp.mean(values * values, axis=-1, keepdims=True)
    return values * lax.rsqrt(mean_sq + NORM_EPS) * gain_row


def causal_blend(rim_rows, local_rows, weights):
    length = local_rows.shape[1]
    padded = jnp.concatenate([rim_rows, local_rows], axis=1).astype(jnp.float32)
    summed_rows = padded[:, 0:length, :] * weights[0]
    for offset in range(1, weights.shape[0]):
        summed_rows = summed_rows + padded[:, offset : offset + length, :] * weights[offset]
    return jax.nn.silu(summed_rows)


def local_pass(scaled_x, keys_b, readout_vectors, log_decay):
    seq_count, seg_len, heads_here = (scaled_x.shape[0], scaled_x.shape[1], scaled_x.shape[2])
    blocks_here = seg_len // BLOCK
    ratio_heads = HEAD_TOTAL // GROUPS

    def to_blocks(tensor):
        return tensor.reshape((seq_count, blocks_here, BLOCK) + tensor.shape[2:])

    x_blocks = to_blocks(scaled_x)
    b_blocks = to_blocks(keys_b)
    c_blocks = to_blocks(readout_vectors)
    inside_block = jnp.cumsum(to_blocks(log_decay), axis=2)
    causal = jnp.tril(jnp.ones((BLOCK, BLOCK), bool))[None, None, :, :, None]
    spread_log = inside_block[:, :, :, None, :] - inside_block[:, :, None, :, :]
    decay_matrix = jnp.where(causal, jnp.exp(jnp.where(causal, spread_log, 0.0)), 0.0)
    scores = jnp.einsum("sblgn,sbtgn->sbltg", c_blocks, b_blocks, precision=PRECISE)
    scores = jnp.repeat(scores, ratio_heads, axis=4)
    key_heads = jnp.repeat(b_blocks, ratio_heads, axis=3)
    query_heads = jnp.repeat(c_blocks, ratio_heads, axis=3)
    inner_part = jnp.einsum(
        "sblth,sbthp->sblhp", scores * decay_matrix, x_blocks, precision=PRECISE
    )
    tail_weight = jnp.exp(inside_block[:, :, -1:, :] - inside_block)
    block_states = jnp.einsum(
        "sblhn,sblhp->sbhpn", key_heads, x_blocks * tail_weight[..., None], precision=PRECISE
    )
    block_totals = inside_block[:, :, -1, :]
    running = jnp.zeros((seq_count, heads_here, HEAD_DIM, STATE), jnp.float32)
    entering = [running]
    running = jnp.exp(block_totals[:, 0])[:, :, None, None] * running + block_states[:, 0]
    entering_states = jnp.stack(entering, axis=1)
    forwarded_portion = jnp.einsum(
        "sblhn,sbhpn->sblhp", query_heads, entering_states, precision=PRECISE
    )
    forwarded_portion = forwarded_portion * jnp.exp(inside_block)[..., None]
    local_out = (inner_part + forwarded_portion).reshape(seq_count, seg_len, heads_here, HEAD_DIM)
    decay_total = jnp.exp(jnp.sum(block_totals, axis=1))
    prefix_log = jnp.cumsum(log_decay, axis=1)
    return (local_out, decay_total, running, prefix_log)


def read_in(local_out, readout_vectors, prefix_log, incoming):
    query_heads = jnp.repeat(readout_vectors, HEAD_TOTAL // GROUPS, axis=2)
    carried = jnp.einsum("slhn,shpn->slhp", query_heads, incoming, precision=PRECISE)
    return local_out + carried * jnp.exp(prefix_log)[..., None]


def combine(preceding_portion, latter):
    return (
        preceding_portion[0] * latter[0],
        latter[0][:, :, None, None] * preceding_portion[1] + latter[1],
    )


def body(
    tokens,
    in_gain,
    gate_weight,
    input_weight,
    key_weight,
    query_weight,
    step_weight,
    conv_input,
    conv_key,
    conv_query,
    step_bias,
    decay_rate,
    decay_extra,
    out_gain,
    out_weight,
):
    normed = rms_rows(tokens.astype(jnp.float32), in_gain).astype(jnp.bfloat16)
    joined_weight = jnp.concatenate(
        [gate_weight, input_weight, key_weight, query_weight, step_weight], axis=1
    )
    token_segment = lax.all_gather(normed, "tp", axis=1, tiled=True)
    seq_count = token_segment.shape[0]
    row_count = token_segment.shape[1]
    result = jnp.dot(
        token_segment.reshape(seq_count * row_count, token_segment.shape[2]),
        joined_weight,
        preferred_element_type=jnp.float32,
    )
    projected = result.astype(jnp.bfloat16).reshape(seq_count, row_count, joined_weight.shape[1])
    seq_count, seg_len = (projected.shape[0], projected.shape[1])
    inner_here = gate_weight.shape[1]
    state_cols = key_weight.shape[1]
    heads_here = step_bias.shape[0]
    gate_in = projected[:, :, :inner_here]
    conv_in = projected[:, :, inner_here : 2 * inner_here + 2 * state_cols]
    step_all = projected[:, :, 2 * inner_here + 2 * state_cols :]
    rim_rows = from_behind(conv_in[:, seg_len - CONV + 1 :, :], "sp", 1)
    conv_weights = jnp.concatenate([conv_input, conv_key, conv_query], axis=1)
    conv_out = causal_blend(rim_rows, conv_in, conv_weights)
    conv_values = conv_out[:, :, :inner_here].reshape(seq_count, seg_len, heads_here, HEAD_DIM)
    keys_b = conv_out[:, :, inner_here : inner_here + state_cols].reshape(
        seq_count, seg_len, state_cols // STATE, STATE
    )
    readout_vectors = conv_out[:, :, inner_here + state_cols :].reshape(
        seq_count, seg_len, state_cols // STATE, STATE
    )
    own_steps = lax.dynamic_slice_in_dim(step_all, lax.axis_index("tp") * heads_here, heads_here, 2)
    step_size = jax.nn.softplus(own_steps.astype(jnp.float32) + step_bias)
    log_decay = -step_size * decay_rate + jnp.transpose(decay_extra, (0, 2, 1))
    scaled_x = conv_values * step_size[..., None]
    local_out, decay_total, final_state, prefix_log = local_pass(
        scaled_x, keys_b, readout_vectors, log_decay
    )
    incoming = carried_in(
        (decay_total, final_state),
        "sp",
        combine,
        (jnp.ones_like(decay_total), jnp.zeros_like(final_state)),
    )
    blended_heads = read_in(local_out, readout_vectors, prefix_log, incoming[1])
    gated_rows = blended_heads.reshape(seq_count, seg_len, inner_here) * jax.nn.silu(
        gate_in.astype(jnp.float32)
    )
    group_width = HEAD_TOTAL // GROUPS * HEAD_DIM
    groups_here = inner_here // group_width
    normed_out = rms_rows(
        gated_rows.reshape(seq_count, seg_len, groups_here, group_width),
        out_gain.reshape(groups_here, group_width),
    )
    normed_out = normed_out.reshape(seq_count, seg_len, inner_here).astype(jnp.bfloat16)
    token_rows = lax.all_to_all(normed_out, "tp", split_axis=1, concat_axis=2, tiled=True)
    result = jnp.dot(
        token_rows.reshape(token_rows.shape[0] * token_rows.shape[1], token_rows.shape[2]),
        out_weight,
        preferred_element_type=jnp.float32,
    )
    return result.astype(jnp.bfloat16).reshape(
        token_rows.shape[0], token_rows.shape[1], out_weight.shape[1]
    )

MESH = pl.DeviceIdType.MESH


def fused_kernel(
    dims,
    tok, gain, gw, iw, kw, qw, sw, cx, ck, cq, sb, dr, de, og, ow,
    out,
    W, SW, OW, tokg, pay, aux, payr, auxr, mix, fin,
    wsem, own_sem, xs, xr, ps, pr, fs, fr, ds, dsa, rs, rsa, ms, mr, round_sem,
):
    nsp, ntp, S, R, D, inner, st, heads = dims
    bf, f32 = jnp.bfloat16, jnp.float32
    width = HEAD_TOTAL // GROUPS * HEAD_DIM
    G = inner // width
    X = ntp // 2
    N = ntp * R
    ratio = HEAD_TOTAL // GROUPS
    sp = lax.axis_index("sp")
    tp = lax.axis_index("tp")
    x, c = tp // 2, tp % 2
    partner = x * 2 + 1 - c
    me = sp * ntp + tp
    total = nsp * ntp

    parts = [
        (gw, W.at[:, 0:inner]),
        (iw, W.at[:, inner : 2 * inner]),
        (kw, W.at[:, 2 * inner : 2 * inner + st]),
        (qw, W.at[:, 2 * inner + st : 2 * inner + 2 * st]),
        (sw, SW),
        (ow, OW),
    ]
    loads = [pltpu.make_async_copy(a, b, wsem.at[i]) for i, (a, b) in enumerate(parts)]
    for load in loads[:5]:
        load.start()
    own = pltpu.make_async_copy(tok, tokg.at[:, tp], own_sem)
    own.start()

    barrier = pltpu.get_barrier_semaphore()

    def near(sem):
        row = sp // G
        for d in range(1, G):
            other = row * G + (sp + d) % G
            pl.semaphore_signal(sem, inc=1, device_id=(other, tp), device_id_type=MESH)

        @pl.when(row > 0)
        def _():
            pl.semaphore_signal(sem, inc=1, device_id=(sp - G, tp), device_id_type=MESH)

        @pl.when(row < S - 1)
        def _():
            pl.semaphore_signal(sem, inc=1, device_id=(sp + G, tp), device_id_type=MESH)

    def near_wait(sem, extra):
        row = sp // G
        ends = jnp.where(row > 0, 1, 0) + jnp.where(row < S - 1, 1, 0)
        pl.semaphore_wait(sem, G - 1 + extra + ends)

    for d in range(1, ntp):
        pl.semaphore_signal(
            barrier, inc=1, device_id=(sp, (tp + d) % ntp), device_id_type=MESH
        )
    near(barrier)
    near_wait(barrier, ntp - 1)

    def seq_of(k):
        return (sp // G + 1 + k) % S

    def cross(k, dx):
        s = seq_of(k)
        return pltpu.make_async_remote_copy(
            src_ref=tok.at[s], dst_ref=tokg.at[s, tp],
            send_sem=xs.at[dx - 1, k], recv_sem=xr.at[dx - 1, k],
            device_id=(sp, (x + dx) % X * 2 + c), device_id_type=MESH,
        )

    def beside(k):
        s = seq_of(k)
        return pltpu.make_async_remote_copy(
            src_ref=tok.at[s], dst_ref=tokg.at[s, tp],
            send_sem=ps.at[k], recv_sem=pr.at[k],
            device_id=(sp, partner), device_id_type=MESH,
        )

    def passed_on(k, dx):
        s = seq_of(k)
        source = (x - dx + X) % X * 2 + c
        return pltpu.make_async_remote_copy(
            src_ref=tokg.at[s, source], dst_ref=tokg.at[s, source],
            send_sem=fs.at[dx - 1, k], recv_sem=fr.at[dx - 1, k],
            device_id=(sp, partner), device_id_type=MESH,
        )

    for k in range(S):
        for dx in range(1, X):
            cross(k, dx).start()
    for k in range(S):
        beside(k).start()
    loads[5].start()
    for i in range(S - 1):
        near(round_sem.at[i])
        near_wait(round_sem.at[i], 0)

    def out_pair(dest):
        args = dict(device_id=(dest, tp), device_id_type=MESH)
        return (
            pltpu.make_async_remote_copy(
                src_ref=pay.at[dest], dst_ref=payr.at[sp],
                send_sem=ds.at[dest], recv_sem=rs.at[sp], **args,
            ),
            pltpu.make_async_remote_copy(
                src_ref=aux.at[dest], dst_ref=auxr.at[sp],
                send_sem=dsa.at[dest], recv_sem=rsa.at[sp], **args,
            ),
        )

    head_id = lax.broadcasted_iota(jnp.int32, (heads, N), 0)
    bias_col = jnp.zeros((heads, N), f32)
    rate_col = jnp.zeros((heads, N), f32)
    for h in range(heads):
        bias_col = jnp.where(head_id == h, sb[h], bias_col)
        rate_col = jnp.where(head_id == h, dr[h], rate_col)

    def project(k):
        s = seq_of(k)
        t = tokg[s].reshape(N, D).astype(f32)
        scale = lax.rsqrt(jnp.mean(t * t, axis=-1, keepdims=True) + NORM_EPS)
        n = (t * scale * gain[...]).astype(bf)
        p = jnp.dot(n, W[...], preferred_element_type=f32)
        steps = lax.dot_general(
            SW[...], n, (((1,), (1,)), ((), ())), preferred_element_type=f32
        )
        steps = steps.astype(bf).astype(f32)
        mine = steps[0:heads]
        for j in range(1, ntp):
            mine = jnp.where(tp == j, steps[j * heads : (j + 1) * heads], mine)
        dt = jax.nn.softplus(mine + bias_col)
        ld = de[s] - dt * rate_col
        for g in range(G):
            dest = s * G + g
            keys = p[:, 2 * inner + g * STATE : 2 * inner + (g + 1) * STATE]
            queries = p[:, 2 * inner + st + g * STATE : 2 * inner + st + (g + 1) * STATE]
            pay[dest, :, 0:width] = p[:, inner + g * width : inner + (g + 1) * width].astype(bf)
            pay[dest, :, width : width + 2 * STATE] = jnp.concatenate(
                [keys, queries], axis=1
            ).astype(bf)
            pay[dest, :, width + 2 * STATE :] = p[:, g * width : (g + 1) * width].astype(bf)
            rows = jnp.concatenate(
                [
                    dt[g * ratio : (g + 1) * ratio],
                    ld[g * ratio : (g + 1) * ratio],
                    jnp.zeros((8 - 2 * ratio, N), f32),
                ],
                axis=0,
            )
            aux[dest] = jnp.concatenate([rows, jnp.zeros((8, 128 - N), f32)], axis=1)

            @pl.when(dest != sp)
            def _():
                for copy in out_pair(dest):
                    copy.start()

            @pl.when(dest == sp)
            def _():
                pltpu.make_async_copy(pay.at[dest], payr.at[sp], rs.at[sp]).start()
                pltpu.make_async_copy(aux.at[dest], auxr.at[sp], rsa.at[sp]).start()

    for load in loads[:5]:
        load.wait()
    own.wait()
    for k in range(S + 1):
        if k < S:
            for dx in range(1, X):
                cross(k, dx).wait_recv()
                passed_on(k, dx).start()
        if k >= 1:
            beside(k - 1).wait_recv()
            for dx in range(1, X):
                passed_on(k - 1, dx).wait_recv()
            project(k - 1)

    g = sp % G
    mine_seq = sp // G
    L = nsp * N

    def pick(make):
        chosen = make(0)
        for j in range(1, G):
            chosen = jnp.where(g == j, make(j), chosen)
        return chosen

    taps = pick(
        lambda j: jnp.concatenate(
            [
                cx[:, j * width : (j + 1) * width],
                ck[:, j * STATE : (j + 1) * STATE],
                cq[:, j * STATE : (j + 1) * STATE],
            ],
            axis=1,
        )
    )
    gain_out = pick(lambda j: og[:, j * width : (j + 1) * width])

    for b in range(nsp):
        pltpu.make_async_copy(auxr.at[b], auxr.at[b], rsa.at[b]).wait()

    A = auxr[...].reshape(nsp * 8, 128)
    upto = lax.broadcasted_iota(jnp.int32, (128, 128), 0) <= lax.broadcasted_iota(
        jnp.int32, (128, 128), 1
    )
    cum = jnp.dot(A, upto.astype(f32), precision=PRECISE, preferred_element_type=f32)
    AT, cumT = A.T, cum.T
    conv_w = width + 2 * STATE
    first_head = lax.broadcasted_iota(jnp.int32, (N, width), 1) < HEAD_DIM
    first_row = lax.broadcasted_iota(jnp.int32, (1, width), 1) < HEAD_DIM
    causal = lax.broadcasted_iota(jnp.int32, (N, N), 0) >= lax.broadcasted_iota(
        jnp.int32, (N, N), 1
    )
    row_id = lax.broadcasted_iota(jnp.int32, (N, conv_w), 0)
    channel = tp * G + g

    def result_copy(b, j):
        return pltpu.make_async_remote_copy(
            src_ref=mix.at[b, j],
            dst_ref=fin.at[mine_seq, :, pl.ds(pl.multiple_of(channel * width, width), width)],
            send_sem=ms.at[b * ntp + j], recv_sem=mr.at[me],
            device_id=(b, j), device_id_type=MESH,
        )

    state = jnp.zeros((STATE, width), f32)
    before = jnp.zeros((N, conv_w), f32)
    for b in range(nsp):
        pltpu.make_async_copy(payr.at[b], payr.at[b], rs.at[b]).wait()
        now = payr[b, :, 0:conv_w].astype(f32)
        acc = now * taps[CONV - 1 : CONV]
        for k in range(1, CONV):
            shifted = jnp.where(row_id < k, pltpu.roll(before, k, 0), pltpu.roll(now, k, 0))
            acc = acc + shifted * taps[CONV - 1 - k : CONV - k]
        before = now
        v = jax.nn.silu(acc)
        kb = v[:, width : width + STATE].astype(bf)
        qb = v[:, width + STATE :].astype(bf)
        r = b * 8
        cols = [cumT[0:N, r + ratio + h : r + ratio + h + 1] for h in range(2)]
        rows = [cum[r + ratio + h : r + ratio + h + 1, 0:N] for h in range(2)]
        tots = [cum[r + ratio + h : r + ratio + h + 1, 127:128] for h in range(2)]
        step = jnp.where(first_head, AT[0:N, r : r + 1], AT[0:N, r + 1 : r + 2])
        reach = jnp.where(first_head, cols[0], cols[1])
        total_row = jnp.where(first_row, tots[0], tots[1])
        xd = v[:, 0:width] * step
        xb = xd.astype(bf)
        scores = lax.dot_general(qb, kb, (((1,), (1,)), ((), ())), preferred_element_type=f32)
        inner_parts = []
        for h in range(2):
            spread = jnp.where(causal, cols[h] - rows[h], 0.0)
            weights = jnp.where(causal, scores * jnp.exp(spread), 0.0).astype(bf)
            inner_parts.append(jnp.dot(weights, xb, preferred_element_type=f32))
        y = jnp.where(first_head, inner_parts[0], inner_parts[1])
        y = y + jnp.dot(qb, state.astype(bf), preferred_element_type=f32) * jnp.exp(reach)
        tail = (xd * jnp.exp(total_row - reach)).astype(bf)
        fresh = lax.dot_general(kb, tail, (((0,), (0,)), ((), ())), preferred_element_type=f32)
        state = jnp.exp(total_row) * state + fresh
        gated = y * jax.nn.silu(payr[b, :, conv_w:].astype(f32))
        scale = lax.rsqrt(jnp.mean(gated * gated, axis=-1, keepdims=True) + NORM_EPS)
        mix[b] = (gated * scale * gain_out).astype(bf).reshape(ntp, R, width)
        for j in range(ntp):
            same = jnp.logical_and(sp == b, tp == j)

            @pl.when(jnp.logical_not(same))
            def _():
                result_copy(b, j).start()

            @pl.when(same)
            def _():
                pltpu.make_async_copy(
                    mix.at[b, j],
                    fin.at[mine_seq, :, pl.ds(pl.multiple_of(channel * width, width), width)],
                    mr.at[me],
                ).start()

    loads[5].wait()
    for i in range(total):
        slot = fin.at[i // ntp // G, :, pl.ds((i % ntp * G + i // ntp % G) * width, width)]
        pltpu.make_async_copy(slot, slot, mr.at[i]).wait()
    rows = fin[...].reshape(S * R, ntp * inner)
    res = jnp.dot(rows, OW[...], preferred_element_type=f32)
    out[...] = res.astype(bf).reshape(S, R, D)

    for k in range(S):
        for dx in range(1, X):
            cross(k, dx).wait_send()
            passed_on(k, dx).wait_send()
        beside(k).wait_send()
    for b in range(nsp):

        @pl.when(b != sp)
        def _():
            for copy in out_pair(b):
                copy.wait_send()

        for j in range(ntp):

            @pl.when(jnp.logical_not(jnp.logical_and(sp == b, tp == j)))
            def _():
                result_copy(b, j).wait_send()


def fused_body(
    nsp, ntp,
    tokens, in_gain, gate_weight, input_weight, key_weight, query_weight, step_weight,
    conv_input, conv_key, conv_query, step_bias, decay_rate, decay_extra, out_gain, out_weight,
):
    S, R, D = tokens.shape
    inner, st, heads = gate_weight.shape[1], key_weight.shape[1], step_bias.shape[0]
    dims = (nsp, ntp, S, R, D, inner, st, heads)
    width = HEAD_TOTAL // GROUPS * HEAD_DIM
    N, X = ntp * R, ntp // 2
    pay_w = 2 * width + 2 * STATE
    bf, f32 = jnp.bfloat16, jnp.float32
    dma = pltpu.SemaphoreType.DMA
    vmem = pl.BlockSpec(memory_space=pltpu.VMEM)
    hbm = pl.BlockSpec(memory_space=pl.ANY)
    smem = pl.BlockSpec(memory_space=pltpu.SMEM)
    return pl.pallas_call(
        functools.partial(fused_kernel, dims),
        out_shape=jax.ShapeDtypeStruct((S, R, out_weight.shape[1]), bf),
        in_specs=[vmem, vmem, hbm, hbm, hbm, hbm, hbm] + [vmem] * 3 + [smem] * 2 + [vmem] * 2 + [hbm],
        out_specs=vmem,
        scratch_shapes=[
            pltpu.VMEM((D, 2 * inner + 2 * st), bf),
            pltpu.VMEM(step_weight.shape[::-1], bf),
            pltpu.VMEM(out_weight.shape, bf),
            pltpu.VMEM((S, ntp, R, D), bf),
            pltpu.VMEM((nsp, N, pay_w), bf),
            pltpu.VMEM((nsp, 8, 128), f32),
            pltpu.VMEM((nsp, N, pay_w), bf),
            pltpu.VMEM((nsp, 8, 128), f32),
            pltpu.VMEM((nsp, ntp, R, width), bf),
            pltpu.VMEM((S, R, ntp * inner), bf),
            dma((6,)),
            dma,
            dma((X - 1, S)), dma((X - 1, S)),
            dma((S,)), dma((S,)),
            dma((X - 1, S)), dma((X - 1, S)),
            dma((nsp,)), dma((nsp,)), dma((nsp,)), dma((nsp,)),
            dma((nsp * ntp,)), dma((nsp * ntp,)),
            pltpu.SemaphoreType.REGULAR((S - 1,)),
        ],
        compiler_params=pltpu.CompilerParams(
            collective_id=0, has_side_effects=True, vmem_limit_bytes=56 * 1024 * 1024
        ),
        name="mixer",
    )(
        tokens, in_gain.reshape(1, -1), gate_weight, input_weight, key_weight, query_weight,
        step_weight.T, conv_input, conv_key, conv_query, step_bias, decay_rate, decay_extra, out_gain.reshape(1, -1), out_weight,
    )


def fits(nsp, ntp, tokens, inner, st, length):
    seqs = tokens[0]
    width = HEAD_TOTAL // GROUPS * HEAD_DIM
    rows = length // (nsp * ntp)
    return (
        ntp % 2 == 0 and ntp > 2 and inner % width == 0 and width == 128
        and 2 * STATE == 128 and HEAD_TOTAL // GROUPS == 2
        and seqs * (inner // width) == nsp and rows % 16 == 0 and rows * ntp == BLOCK
    )


def solution(mesh):
    placed = (
        P(None, ("sp", "tp"), None),
        P(),
        P(None, "tp"),
        P(None, "tp"),
        P(None, "tp"),
        P(None, "tp"),
        P(),
        P(None, "tp"),
        P(None, "tp"),
        P(None, "tp"),
        P("tp"),
        P("tp"),
        P(None, "tp", "sp"),
        P("tp"),
        P(),
    )
    nsp, ntp = mesh.shape["sp"], mesh.shape["tp"]

    def chosen(*args):
        inner, st = args[2].shape[1], args[4].shape[1]
        rows = args[0].shape[1] * nsp * ntp
        if fits(nsp, ntp, args[0].shape, inner, st, rows):
            return fused_body(nsp, ntp, *args)
        return body(*args)

    return jax.shard_map(
        chosen, mesh=mesh, in_specs=placed, out_specs=P(None, ("sp", "tp"), None), check_vma=False
    )
```
